32 devices in a mesh: fs: 8 (over z, y), tp: 4 (over x, core).
Axes of the slice: x: 2, y: 2, z: 4, core: 2. Of those that a mesh axis runs over, the one named last changes fastest.
Arguments:
- tokens: bfloat16 [8192, 2048], P('fs', 'tp'), may hold values from -40 to 40
- first_gain: float32 [2048], replicated, may hold values from 0.1 to 1.9
- first_gate: bfloat16 [2048, 6144], P('fs', 'tp'), may hold values from -0.125 to 0.125
- first_upward: bfloat16 [2048, 6144], P('fs', 'tp'), may hold values from -0.125 to 0.125
- first_down: bfloat16 [6144, 2048], P('tp', 'fs'), may hold values from -0.078125 to 0.078125
- mix_gain: float32 [2048], replicated, may hold values from 0.1 to 1.9
- mix_input: bfloat16 [2048, 1024], P('fs', 'tp'), may hold values from -0.125 to 0.125
- pool_weight: bfloat16 [8, 128, 128], replicated, may hold values from -0.5 to 0.5
- pool_scale: float32 [1024], replicated, may hold values from 0.1 to 1.9
- mix_output: bfloat16 [1024, 2048], P('tp', 'fs'), may hold values from -0.1875 to 0.1875
- second_gain: float32 [2048], replicated, may hold values from 0.1 to 1.9
- second_gate: bfloat16 [2048, 6144], P('fs', 'tp'), may hold values from -0.125 to 0.125
- second_upward: bfloat16 [2048, 6144], P('fs', 'tp'), may hold values from -0.125 to 0.125
- second_down: bfloat16 [6144, 2048], P('tp', 'fs'), may hold values from -0.078125 to 0.078125
Outputs:
- layer_out: bfloat16 [8192, 2048], P('fs', 'tp')
The draws below stay inside these ranges and needn't reach their ends.
All inputs are finite; a program needn't handle non-finite values.
Results may differ from the reference program's by a relative error of at most 0.01.
Values may be sent and summed in bfloat16 or wider, within the bound.
No kernel may reach another device: no remote copies, remote signals or barrier semaphores. Data moves between devices by JAX's collectives and lax.ppermute only.
A program may use at most 128 MiB of HBM per device.

```python
import math
import jax
import jax.numpy as jnp
from jax import lax

D = 2048
FF = 6144
GROUPS = 8
GROUP_DIM = 128
TOK_DEV = 1024
POOL_WIDTH = 1024
TOKENS = 8192
N_FS = 8
N_TP = 4


def draw_tokens(key, part):
    keys = jax.random.split(jax.random.fold_in(key, 11), 3)
    base = jax.random.normal(keys[0], (TOKENS, D), jnp.float32)
    base = jnp.clip(base, -4.0, 4.0)
    row_scale = jnp.exp(jax.random.uniform(keys[1], (TOKENS, 1), jnp.float32, math.log(0.5), math.log(5.0)))
    col_scale = jnp.exp(jax.random.uniform(keys[2], (1, D), jnp.float32, math.log(0.5), math.log(2.0)))
    return (base * row_scale * col_scale).astype(jnp.bfloat16)


def shard_levels(stream_key, shape, shards, low, high):
    gain, own = 1.0, jax.random.fold_in(stream_key, 6)
    for axis_at, blocks in shards:
        draws = jnp.exp(jax.random.uniform(jax.random.fold_in(own, axis_at), (blocks,), jnp.float32, low / len(shards), high / len(shards)))
        gain = gain * jnp.repeat(draws, shape[axis_at] // blocks).reshape([-1 if axis == axis_at else 1 for axis in range(len(shape))])
    return gain


def normal_values(key, dims, scale, limit, shards=(), kind=jnp.bfloat16):
    values = scale * jax.random.normal(key, dims, jnp.float32)
    if shards:
        values = values * shard_levels(key, dims, shards, -0.22, 0.18)
    return jnp.clip(values, -limit, limit).astype(kind)


def setup_inputs(seed: int = 0) -> dict:
    streams_of = jax.random.split(jax.random.key(seed), 15)
    tokens = draw_tokens(jax.random.fold_in(streams_of[14], 71), 0)
    first_gain = jnp.clip(1.0 + 0.18 * jax.random.normal(streams_of[1], (D,), jnp.float32), 0.1, 1.9)
    first_gate = normal_values(streams_of[2], (D, FF), D ** -0.5, 0.125, ((0, 8), (1, 4)))
    first_upward = normal_values(streams_of[3], (D, FF), D ** -0.5, 0.125, ((0, 8), (1, 4)))
    first_down = normal_values(streams_of[4], (FF, D), FF ** -0.5, 0.078125, ((0, 4), (1, 8)))
    mix_gain = jnp.clip(1.0 + 0.18 * jax.random.normal(streams_of[5], (D,), jnp.float32), 0.1, 1.9)
    mix_input = normal_values(streams_of[6], (D, POOL_WIDTH), D ** -0.5, 0.125, ((0, 8), (1, 4)))
    pool_weight = normal_values(streams_of[7], (GROUPS, GROUP_DIM, GROUP_DIM), GROUP_DIM ** -0.5, 0.5)
    pool_scale = jnp.clip(1.0 + 0.18 * jax.random.normal(streams_of[8], (POOL_WIDTH,), jnp.float32), 0.1, 1.9)
    mix_output = normal_values(streams_of[9], (POOL_WIDTH, D), POOL_WIDTH ** -0.5, 0.1875, ((0, 4), (1, 8)))
    second_gain = jnp.clip(1.0 + 0.18 * jax.random.normal(streams_of[10], (D,), jnp.float32), 0.1, 1.9)
    second_gate = normal_values(streams_of[11], (D, FF), D ** -0.5, 0.125, ((0, 8), (1, 4)))
    second_upward = normal_values(streams_of[12], (D, FF), D ** -0.5, 0.125, ((0, 8), (1, 4)))
    second_down = normal_values(streams_of[13], (FF, D), FF ** -0.5, 0.078125, ((0, 4), (1, 8)))
    return {"tokens": tokens, "first_gain": first_gain, "first_gate": first_gate, "first_upward": first_upward, "first_down": first_down, "mix_gain": mix_gain, "mix_input": mix_input, "pool_weight": pool_weight, "pool_scale": pool_scale, "mix_output": mix_output, "second_gain": second_gain, "second_gate": second_gate, "second_upward": second_upward, "second_down": second_down}


EPSILON = 1e-06
REACH = 15

def normalize(values, weight_gain):
    wide = values.astype(jnp.float32)
    factor = lax.rsqrt(lax.optimization_barrier(jnp.mean(wide * wide, axis=-1, keepdims=True)) + EPSILON)
    return (wide * factor * weight_gain).astype(jnp.bfloat16)

def block_sum(left, right):
    width = left.shape[1] // N_TP
    summed = jnp.zeros((left.shape[0], right.shape[1]), jnp.float32)
    for block in range(N_TP):
        piece = jnp.dot(left[:, block * width:(block + 1) * width], right[block * width:(block + 1) * width], preferred_element_type=jnp.float32)
        summed = summed + lax.optimization_barrier(piece.astype(jnp.bfloat16)).astype(jnp.float32)
    return summed

def feed_forward(values, weight_gain, gate_weight, upward_weight, down_weight):
    normed = normalize(values, weight_gain)
    gated = jnp.dot(normed, gate_weight, preferred_element_type=jnp.float32)
    upward = jnp.dot(normed, upward_weight, preferred_element_type=jnp.float32)
    hidden = (jax.nn.silu(gated) * upward).astype(jnp.bfloat16)
    summed = block_sum(hidden, down_weight)
    return (values.astype(jnp.float32) + 0.5 * summed).astype(jnp.bfloat16)

def pool_mixer(values, mix_gain, mix_input, pool_weight, pool_scale, mix_output):
    normed = normalize(values, mix_gain)
    pool_in = jnp.dot(normed, mix_input, preferred_element_type=jnp.float32).astype(jnp.bfloat16)
    width = pool_in.shape[1]
    sequences = pool_in.reshape(N_FS, TOK_DEV, width).astype(jnp.float32)
    padded = jnp.pad(sequences, ((0, 0), (REACH, 0), (0, 0)))
    windows = jnp.left_shift(2, jnp.arange(GROUPS, dtype=jnp.int32) % 4)
    window_cols = jnp.repeat(windows, GROUP_DIM)[None, None, :]
    summed = jnp.zeros(sequences.shape, jnp.float32)
    for offset in range(REACH + 1):
        shifted = padded[:, REACH - offset:REACH - offset + TOK_DEV]
        summed = summed + jnp.where(offset < window_cols, shifted, 0.0)
    positions = jnp.arange(TOK_DEV, dtype=jnp.int32)
    counts = jnp.minimum(positions[None, :, None] + 1, window_cols).astype(jnp.float32)
    pooled = (summed / counts - sequences).astype(jnp.bfloat16).reshape(TOKENS, GROUPS, GROUP_DIM)
    mapped = jnp.einsum('tgc,gcd->tgd', pooled.astype(jnp.float32), pool_weight.astype(jnp.float32))
    mapped = (mapped.reshape(TOKENS, width) * pool_scale).astype(jnp.bfloat16)
    mixer = block_sum(mapped, mix_output)
    return (values.astype(jnp.float32) + mixer).astype(jnp.bfloat16)

def reference(tokens, first_gain, first_gate, first_upward, first_down, mix_gain, mix_input, pool_weight, pool_scale, mix_output, second_gain, second_gate, second_upward, second_down):
    first_out = feed_forward(tokens, first_gain, first_gate, first_upward, first_down)
    mid_out = pool_mixer(first_out, mix_gain, mix_input, pool_weight, pool_scale, mix_output)
    return feed_forward(mid_out, second_gain, second_gate, second_upward, second_down)
```

```python
import functools
import jax
import jax.numpy as jnp
from jax import lax
from jax.experimental import pallas as pl
from jax.experimental.pallas import tpu as pltpu
from jax.sharding import PartitionSpec as P

GROUP_DIM = 128
EPSILON = 1e-06
REACH = 15
CORES = 2
CHUNKS = 2
AXES = ("fs", "tp")


class Grid:
    def __init__(self, mesh):
        self.fs, self.tp = mesh.shape["fs"], mesh.shape["tp"]
        self.nx = self.tp // CORES
        self.ny = self.nx
        self.nzh = self.fs // (CORES * self.ny)

    def place(self):
        fs, tp = lax.axis_index("fs"), lax.axis_index("tp")
        y, z = fs % self.ny, fs // self.ny
        return z // CORES, z % CORES, y, tp // CORES, tp % CORES

    def permute(self, value, target):
        pairs = []
        for source in range(self.fs * self.tp):
            fs, tp = divmod(source, self.tp)
            z, y = divmod(fs, self.ny)
            to = target(z // CORES, z % CORES, y, tp // CORES, tp % CORES)
            if to is not None:
                zh, zl, y, x, c = to
                pairs.append((source, ((zh * CORES + zl) * self.ny + y) * self.tp + x * CORES + c))
        return lax.ppermute(value, AXES, pairs)

    def shift_x(self, value, i):
        return self.permute(value, lambda zh, zl, y, x, c: (zh, zl, y, (x + i) % self.nx, c))

    def flip_zl(self, value):
        return self.permute(value, lambda zh, zl, y, x, c: (zh, 1 - zl, y, x, c))

    def flip_core(self, value):
        return self.permute(value, lambda zh, zl, y, x, c: (zh, zl, y, x, 1 - c))

    def gather_weight(self, shard):
        lines = []
        for i in range(self.nzh):
            lines.append(
                self.permute(shard, lambda zh, zl, y, x, c: ((zh + i) % self.nzh, c, y, x, zl))
            )
        planes = list(lines)
        for j in range(1, self.ny):
            for value in lines:
                planes.append(
                    self.permute(value, lambda zh, zl, y, x, c: (zh, zl, (y + j) % self.ny, x, c))
                )
        return planes + [self.flip_core(value) for value in planes]

    def slots(self):
        zh, _, y, _, c = self.place()
        found = []
        for k in range(CORES):
            for j in range(self.ny):
                for i in range(self.nzh):
                    z = (zh - i) % self.nzh * CORES + (c + k) % CORES
                    found.append(z * self.ny + (y - j) % self.ny)
        return jnp.stack(found).astype(jnp.int32)


def normalize(values, weight_gain):
    wide = values.astype(jnp.float32)
    factor = lax.rsqrt(jnp.mean(wide * wide, axis=-1, keepdims=True) + EPSILON)
    return (wide * factor * weight_gain).astype(jnp.bfloat16)


def hidden_kernel(count, depth, slot_ref, values_ref, *refs):
    gates, upwards = refs[:count], refs[count : 2 * count]
    out_ref, gate_ref, upward_ref = refs[2 * count :]
    for at in range(count):
        start = pl.multiple_of(slot_ref[at] * depth, depth)
        gate_ref[pl.ds(start, depth), :] = gates[at][...]
        upward_ref[pl.ds(start, depth), :] = upwards[at][...]
    values = values_ref[...]
    gated = jnp.dot(values, gate_ref[...], preferred_element_type=jnp.float32)
    upward = jnp.dot(values, upward_ref[...], preferred_element_type=jnp.float32)
    out_ref[...] = (gated / (1.0 + jnp.exp(-gated)) * upward).astype(jnp.bfloat16)


def hidden_units(values, slots, pairs, tile=256):
    rows, depth = values.shape
    count, width = len(pairs), pairs[0].shape[1]
    block = depth // count
    gate_spec = pl.BlockSpec((block, tile), lambda j, s: (0, j))
    upward_spec = pl.BlockSpec((block, tile), lambda j, s: (1, j))
    return pl.pallas_call(
        functools.partial(hidden_kernel, count, block),
        out_shape=jax.ShapeDtypeStruct((rows, width), jnp.bfloat16),
        grid_spec=pltpu.PrefetchScalarGridSpec(
            num_scalar_prefetch=1,
            grid=(width // tile,),
            in_specs=[pl.BlockSpec((rows, depth), lambda j, s: (0, 0))]
            + [gate_spec] * count
            + [upward_spec] * count,
            out_specs=pl.BlockSpec((rows, tile), lambda j, s: (0, j)),
            scratch_shapes=[pltpu.VMEM((depth, tile), jnp.bfloat16)] * 2,
        ),
        cost_estimate=pl.CostEstimate(
            flops=4 * rows * depth * width,
            bytes_accessed=4 * depth * width + 2 * rows * (depth + width),
            transcendentals=rows * width,
        ),
        name="hidden_units",
    )(slots, values, *pairs, *pairs)


def down_kernel(count, width, slot_ref, hidden_ref, *refs):
    out_ref = refs[count]
    hidden = hidden_ref[...]
    for at in range(count):
        start = pl.multiple_of(slot_ref[at] * width, width)
        piece = jnp.dot(hidden, refs[at][...], preferred_element_type=jnp.float32)
        out_ref[:, pl.ds(start, width)] = piece.astype(jnp.bfloat16)


def down_product(hidden, slots, downs, tile=256):
    rows, depth = hidden.shape
    count, width = len(downs), downs[0].shape[1]
    return pl.pallas_call(
        functools.partial(down_kernel, count, width),
        out_shape=jax.ShapeDtypeStruct((rows, count * width), jnp.bfloat16),
        grid_spec=pltpu.PrefetchScalarGridSpec(
            num_scalar_prefetch=1,
            grid=(rows // tile,),
            in_specs=[pl.BlockSpec((tile, depth), lambda j, s: (j, 0))]
            + [pl.BlockSpec((depth, width), lambda j, s: (0, 0))] * count,
            out_specs=pl.BlockSpec((tile, count * width), lambda j, s: (j, 0)),
        ),
        cost_estimate=pl.CostEstimate(
            flops=2 * rows * depth * count * width,
            bytes_accessed=2 * depth * count * width + 2 * rows * (depth + count * width),
            transcendentals=0,
        ),
        name="down_product",
    )(slots, hidden, *downs)


def feed_forward(values, weight_gain, slots, pairs, downs):
    return down_product(hidden_units(normalize(values, weight_gain), slots, pairs), slots, downs)


def pool_groups(extended, positions, pool_weight, pool_scale):
    row_count = positions.shape[0]
    group_count = extended.shape[1] // GROUP_DIM
    group_ids = jnp.arange(group_count, dtype=jnp.int32)
    windows = jnp.left_shift(2, group_ids % 4)
    window_cols = jnp.repeat(windows, GROUP_DIM)[None, :]
    wide = extended.astype(jnp.float32)
    summed = jnp.zeros((row_count, wide.shape[1]), jnp.float32)
    for offset in range(REACH + 1):
        shifted = wide[REACH - offset : REACH - offset + row_count]
        summed = summed + jnp.where(offset < window_cols, shifted, 0.0)
    counts = jnp.minimum(positions[:, None] + 1, window_cols).astype(jnp.float32)
    pooled = (summed / counts - wide[REACH:]).astype(jnp.bfloat16)
    mapped = jnp.einsum(
        "tgc,gcd->tgd",
        pooled.reshape(row_count, group_count, GROUP_DIM),
        pool_weight,
        preferred_element_type=jnp.float32,
    )
    return (mapped.reshape(row_count, group_count * GROUP_DIM) * pool_scale).astype(jnp.bfloat16)


def per_device(
    grid,
    tokens,
    first_gain,
    first_gate,
    first_upward,
    first_down,
    mix_gain,
    mix_input,
    pool_weight,
    pool_scale,
    mix_output,
    second_gain,
    second_gate,
    second_upward,
    second_down,
):
    zh, zl, y, x, c = grid.place()
    nx, run = grid.nx, x * CORES + zl
    slots = grid.slots()
    length, part = tokens.shape
    width = part * grid.tp

    near = [
        grid.permute(tokens, lambda zh, zl, y, x, c, k=k: (zh, c ^ k, y, x, zl))
        for k in range(CORES)
    ]
    values = jnp.zeros((length, width), jnp.bfloat16)
    for i in range(nx):
        for k in range(CORES):
            piece = grid.shift_x(near[k], i) if i else near[k]
            at = (x - i) % nx * CORES + (zl ^ k)
            values = lax.dynamic_update_slice(values, piece, (0, at * part))

    first_pairs = grid.gather_weight(jnp.concatenate([first_gate, first_upward], 0))
    first_downs = grid.gather_weight(first_down)
    second_pairs = grid.gather_weight(jnp.concatenate([second_gate, second_upward], 0))
    second_downs = grid.gather_weight(second_down)
    input_rows, output_cols = (
        lax.all_gather(mix_input, "fs", axis=0, tiled=True),
        lax.all_gather(mix_output, "fs", axis=1, tiled=True),
    )
    full_input, full_output = (
        lax.all_gather(input_rows, "tp", axis=1, tiled=True),
        lax.all_gather(output_cols, "tp", axis=0, tiled=True),
    )

    chunk = length // CHUNKS
    rows = chunk // grid.tp
    before = jnp.zeros((REACH, full_input.shape[1]), jnp.bfloat16)
    middles = []
    for h in range(CHUNKS):
        own = lax.slice_in_dim(values, h * chunk, (h + 1) * chunk, axis=0)
        parts = feed_forward(own, first_gain, slots, first_pairs, first_downs)
        take = lambda i: lax.dynamic_slice(
            parts, ((x + i) % nx * CORES * rows, 0), (CORES * rows, width)
        )
        total = take(0).astype(jnp.float32)
        for i in range(1, nx):
            total = total + grid.shift_x(take(i), i).astype(jnp.float32)
        half = lambda k: lax.dynamic_slice(total, ((zl ^ k) * rows, 0), (rows, width))
        total = half(0) + grid.flip_zl(half(1).astype(jnp.bfloat16)).astype(jnp.float32)
        residual = lax.dynamic_slice(own, (run * rows, 0), (rows, width))
        first_out = (residual.astype(jnp.float32) + 0.5 * total).astype(jnp.bfloat16)

        normed = normalize(first_out, mix_gain)
        pool_in = jnp.dot(normed, full_input, preferred_element_type=jnp.float32)
        pool_in = pool_in.astype(jnp.bfloat16)

        def next_run(zh, zl, y, x, c):
            to = (x * CORES + zl + 1) % grid.tp
            return zh, to % CORES, y, to // CORES, c

        tail = grid.permute(pool_in[rows - REACH :], next_run)
        extended = jnp.concatenate([jnp.where(run == 0, before, tail), pool_in], 0)
        before = tail
        positions = h * chunk + run * rows + jnp.arange(rows, dtype=jnp.int32)
        mapped = pool_groups(extended, positions, pool_weight, pool_scale)
        mixer = jnp.dot(mapped, full_output, preferred_element_type=jnp.float32)
        mid_out = (first_out.astype(jnp.float32) + mixer).astype(jnp.bfloat16)

        near = [mid_out, grid.flip_zl(mid_out)]
        middle = jnp.zeros((chunk, width), jnp.bfloat16)
        for i in range(nx):
            for k in range(CORES):
                piece = grid.shift_x(near[k], i) if i else near[k]
                at = (x - i) % nx * CORES + (zl ^ k)
                middle = lax.dynamic_update_slice(middle, piece, (at * rows, 0))
        middles.append(middle)

    outs = []
    for middle in middles:
        parts = feed_forward(middle, second_gain, slots, second_pairs, second_downs)
        span = width // nx
        take = lambda value, i: lax.dynamic_slice(
            value, (0, (x + i) % nx * span), (chunk, span)
        )
        total = take(parts, 0).astype(jnp.float32)
        for i in range(1, nx):
            total = total + grid.shift_x(take(parts, i), i).astype(jnp.float32)
        other = grid.permute(
            total.astype(jnp.bfloat16),
            lambda zh, zl, y, x, c: (zh, c, y, x, c) if zl != c else None,
        )
        total = total + other.astype(jnp.float32)
        done = (take(middle, 0).astype(jnp.float32) + 0.5 * total).astype(jnp.bfloat16)
        mine = lax.dynamic_slice(done, (0, c * part), (chunk, part))
        passed = grid.flip_core(lax.dynamic_slice(done, (0, (1 - c) * part), (chunk, part)))
        outs.append(jnp.where(zl == c, mine, passed))
    return jnp.concatenate(outs, 0)


def solution(mesh):
    in_specs = (
        P("fs", "tp"),
        P(),
        P("fs", "tp"),
        P("fs", "tp"),
        P("tp", "fs"),
        P(),
        P("fs", "tp"),
        P(),
        P(),
        P("tp", "fs"),
        P(),
        P("fs", "tp"),
        P("fs", "tp"),
        P("tp", "fs"),
    )
    return jax.shard_map(
        functools.partial(per_device, Grid(mesh)),
        mesh=mesh,
        in_specs=in_specs,
        out_specs=P("fs", "tp"),
        check_vma=False,
    )
```

```python
import functools
import jax
import jax.numpy as jnp
from jax import lax
from jax.experimental import pallas as pl
from jax.experimental.pallas import tpu as pltpu
from jax.sharding import PartitionSpec as P


GROUP_DIM = 128
EPSILON = 1e-06
HALO = 16
CORES = 2
CHUNKS = 2
AXES = ("fs", "tp")


class Grid:
    def __init__(self, mesh):
        self.fs, self.tp = mesh.shape["fs"], mesh.shape["tp"]
        self.nx = self.tp // CORES
        self.ny = self.nx
        self.nzh = self.fs // (CORES * self.ny)

    def place(self):
        fs, tp = lax.axis_index("fs"), lax.axis_index("tp")
        y, z = fs % self.ny, fs // self.ny
        return z // CORES, z % CORES, y, tp // CORES, tp % CORES

    def permute(self, value, target):
        pairs, stay = [], False
        for source in range(self.fs * self.tp):
            fs, tp = divmod(source, self.tp)
            z, y = divmod(fs, self.ny)
            to = target(z // CORES, z % CORES, y, tp // CORES, tp % CORES)
            if to is not None:
                zh, zl, y, x, c = to
                goal = ((zh * CORES + zl) * self.ny + y) * self.tp + x * CORES + c
                stay = stay or goal == source
                if goal != source:
                    pairs.append((source, goal))
        moved = lax.ppermute(value, AXES, pairs)
        if stay:
            here = self.place()
            same = [a == b for a, b in zip(target(*here), here)]
            moved = jnp.where(functools.reduce(jnp.logical_and, same), value, moved)
        return moved

    def shift_x(self, value, i):
        return self.permute(value, lambda zh, zl, y, x, c: (zh, zl, y, (x + i) % self.nx, c))

    def shift_y(self, value, j):
        return self.permute(value, lambda zh, zl, y, x, c: (zh, zl, (y + j) % self.ny, x, c))

    def flip_zl(self, value):
        return self.permute(value, lambda zh, zl, y, x, c: (zh, 1 - zl, y, x, c))

    def flip_core(self, value):
        return self.permute(value, lambda zh, zl, y, x, c: (zh, zl, y, x, 1 - c))

    def gather_lines(self, shard):
        return [
            self.permute(shard, lambda zh, zl, y, x, c: ((zh + i) % self.nzh, c, y, x, zl))
            for i in range(self.nzh)
        ]

    def gather_weight(self, shard):
        lines = self.gather_lines(shard)
        planes = list(lines)
        for j in range(1, self.ny):
            for value in lines:
                planes.append(self.shift_y(value, j))
        return planes + [self.flip_core(value) for value in planes]

    def gather_mixer(self, mix_input, mix_output):
        zh, zl, y, x, c = self.place()
        nzh, nx, ny = self.nzh, self.nx, self.ny
        value = jnp.stack([mix_input, mix_output])
        value = stacked(self.gather_lines(value), [(zh - i) % nzh for i in range(nzh)])
        value = stacked([value, self.flip_zl(value)], [zl, 1 - zl])
        value = value.transpose(2, 0, 1, 3, 4)
        inward = [value[0]] + [self.shift_y(value[0], j) for j in range(1, ny)]
        inward = stacked(inward, [(y - j) % ny for j in range(ny)])
        outward = [value[1]] + [self.shift_x(value[1], i) for i in range(1, nx)]
        outward = stacked(outward, [(x - i) % nx for i in range(nx)])
        inward = [inward] + [self.shift_x(inward, i) for i in range(1, nx)]
        outward = [outward] + [self.shift_y(outward, j) for j in range(1, ny)]
        table = [(x - i) % nx for i in range(nx)] + [(y - j) % ny for j in range(ny)]
        inward += [self.flip_core(v) for v in inward]
        outward += [self.flip_core(v) for v in outward]
        return inward, outward, table + [c]

    def slots(self):
        zh, _, y, _, c = self.place()
        found = []
        for k in range(CORES):
            for j in range(self.ny):
                for i in range(self.nzh):
                    z = (zh - i) % self.nzh * CORES + (c + k) % CORES
                    found.append(z * self.ny + (y - j) % self.ny)
        return jnp.stack(found).astype(jnp.int32)


def stacked(pieces, places):
    full = jnp.stack([pieces[0]] * len(pieces))
    for piece, place in zip(pieces[1:], places[1:]):
        full = lax.dynamic_update_slice(full, piece[None], (place,) + (0,) * piece.ndim)
    return full


def normalize(values, weight_gain):
    wide = values.astype(jnp.float32)
    factor = lax.rsqrt(jnp.mean(wide * wide, axis=-1, keepdims=True) + EPSILON)
    return (wide * factor * weight_gain).astype(jnp.bfloat16)


def hidden_kernel(count, depth, parts, axis, table_ref, gain_ref, *refs):
    pieces, refs = refs[:parts], refs[parts:]
    gates, upwards = refs[:count], refs[count : 2 * count]
    out_ref, values_ref, gate_ref, upward_ref, normed_ref = refs[2 * count :]

    @pl.when(pl.program_id(0) == 0)
    def _():
        for n, piece in enumerate(pieces):
            size = piece.shape[axis]
            start = pl.multiple_of(table_ref[count + n] * size, size)
            if axis:
                values_ref[:, pl.ds(start, size)] = piece[...]
            else:
                values_ref[pl.ds(start, size), :] = piece[...]
        normed_ref[...] = normalize(values_ref[...], gain_ref[...])

    for at in range(count):
        start = pl.multiple_of(table_ref[at] * depth, depth)
        gate_ref[pl.ds(start, depth), :] = gates[at][...]
        upward_ref[pl.ds(start, depth), :] = upwards[at][...]
    values = normed_ref[...]
    gated = jnp.dot(values, gate_ref[...], preferred_element_type=jnp.float32)
    upward = jnp.dot(values, upward_ref[...], preferred_element_type=jnp.float32)
    out_ref[...] = (gated / (1.0 + jnp.exp(-gated)) * upward).astype(jnp.bfloat16)


def hidden_units(table, pieces, piece_shape, piece_row, axis, weight_gain, pairs):
    count, width = len(pairs), pairs[0].shape[1]
    depth = weight_gain.shape[0]
    rows = piece_shape[0] * (1 if axis else len(pieces))
    tile = min(width, 512) if width % 512 == 0 else 256
    block = depth // count
    piece_spec = pl.BlockSpec(piece_shape, lambda j, s: (piece_row, 0))
    gate_spec = pl.BlockSpec((block, tile), lambda j, s: (0, j))
    upward_spec = pl.BlockSpec((block, tile), lambda j, s: (1, j))
    return pl.pallas_call(
        functools.partial(hidden_kernel, count, block, len(pieces), axis),
        out_shape=(
            jax.ShapeDtypeStruct((rows, width), jnp.bfloat16),
            jax.ShapeDtypeStruct((rows, depth), jnp.bfloat16),
        ),
        grid_spec=pltpu.PrefetchScalarGridSpec(
            num_scalar_prefetch=1,
            grid=(width // tile,),
            in_specs=[pl.BlockSpec((1, depth), lambda j, s: (0, 0))]
            + [piece_spec] * len(pieces)
            + [gate_spec] * count
            + [upward_spec] * count,
            out_specs=(
                pl.BlockSpec((rows, tile), lambda j, s: (0, j)),
                pl.BlockSpec((rows, depth), lambda j, s: (0, 0)),
            ),
            scratch_shapes=[pltpu.VMEM((depth, tile), jnp.bfloat16)] * 2
            + [pltpu.VMEM((rows, depth), jnp.bfloat16)],
        ),
        cost_estimate=pl.CostEstimate(
            flops=4 * rows * depth * width,
            bytes_accessed=4 * depth * width + 2 * rows * (2 * depth + width),
            transcendentals=rows * width,
        ),
        name="hidden_units",
    )(table, weight_gain[None], *pieces, *pairs, *pairs)


def down_kernel(count, width, spans, slot_ref, hidden_ref, *refs):
    downs, out_ref = refs[:count], refs[count]
    hidden = hidden_ref[...]
    per = count // spans
    for at in range(count):
        piece = jnp.dot(hidden, downs[at][...], preferred_element_type=jnp.float32)
        column = slot_ref[at]
        start = pl.multiple_of(column % per * width, width)
        place = (column // per + spans - slot_ref[count]) % spans
        out_ref[place, :, pl.ds(start, width)] = piece.astype(jnp.bfloat16)


def down_product(table, hidden, downs, spans=1, tile=256):
    rows, depth = hidden.shape
    count, width = len(downs), downs[0].shape[1]
    span = count * width // spans
    return pl.pallas_call(
        functools.partial(down_kernel, count, width, spans),
        out_shape=jax.ShapeDtypeStruct((spans, rows, span), jnp.bfloat16),
        grid_spec=pltpu.PrefetchScalarGridSpec(
            num_scalar_prefetch=1,
            grid=(rows // tile,),
            in_specs=[pl.BlockSpec((tile, depth), lambda j, s: (j, 0))]
            + [pl.BlockSpec((depth, width), lambda j, s: (0, 0))] * count,
            out_specs=pl.BlockSpec((spans, tile, span), lambda j, s: (0, j, 0)),
        ),
        cost_estimate=pl.CostEstimate(
            flops=2 * rows * depth * count * width,
            bytes_accessed=2 * depth * count * width + 2 * rows * (depth + count * width),
            transcendentals=0,
        ),
        name="down_product",
    )(table, hidden, *downs)


def marked(table):
    def copy(source, target):
        for n in range(table.shape[0]):
            target[n] = source[n]

    spec = pl.BlockSpec(memory_space=pltpu.SMEM)
    return pl.pallas_call(
        copy,
        out_shape=jax.ShapeDtypeStruct(table.shape, table.dtype),
        in_specs=[spec],
        out_specs=spec,
        name="mark",
    )(table)


def mixer_kernel(grid, place_ref, values_ref, total_ref, other_ref, gain_ref, *refs):
    nx, ny = grid.nx, grid.ny
    inward, refs = refs[: CORES * nx], refs[CORES * nx :]
    outward, refs = refs[: CORES * ny], refs[CORES * ny :]
    pool_ref, scale_ref, result_ref, in_full, out_full, mapped_ref = refs
    rows = result_ref.shape[0]
    core = place_ref[2 + nx + ny]
    for k in range(CORES):
        c = core + k - 2 * core * k
        for zl in range(CORES):
            for zh in range(grid.nzh):
                for y in range(ny):
                    for i in range(nx):
                        piece = inward[k * nx + i][y, zl, zh]
                        at = ((zh * CORES + c) * ny + y) * piece.shape[0]
                        to = (place_ref[2 + i] * CORES + zl) * piece.shape[1]
                        at = pl.multiple_of(at, piece.shape[0])
                        to = pl.multiple_of(to, piece.shape[1])
                        in_full[pl.ds(at, piece.shape[0]), pl.ds(to, piece.shape[1])] = piece
                for x in range(nx):
                    for j in range(ny):
                        piece = outward[k * ny + j][x, zl, zh]
                        at = (x * CORES + zl) * piece.shape[0]
                        to = ((zh * CORES + c) * ny + place_ref[2 + nx + j]) * piece.shape[1]
                        to = pl.multiple_of(to, piece.shape[1])
                        out_full[at : at + piece.shape[0], pl.ds(to, piece.shape[1])] = piece
    half = pl.multiple_of(place_ref[1] * rows, rows)
    total = total_ref[pl.ds(half, rows + HALO), :] + other_ref[...].astype(jnp.float32)
    values = (values_ref[...].astype(jnp.float32) + 0.5 * total).astype(jnp.bfloat16)
    pool_in = jnp.dot(
        normalize(values, gain_ref[...]), in_full[...], preferred_element_type=jnp.float32
    )
    pool_in = pool_in.astype(jnp.bfloat16).astype(jnp.float32)
    at = place_ref[0] - HALO + lax.broadcasted_iota(jnp.int32, (rows + HALO, GROUP_DIM), 0)
    for group in range(pool_in.shape[1] // GROUP_DIM):
        cols = slice(group * GROUP_DIM, (group + 1) * GROUP_DIM)
        window = 2 ** (1 + group % 4)
        own = jnp.where(at >= 0, pool_in[:, cols], 0.0)
        summed, step = own, 1
        while step < window:
            summed = summed + pltpu.roll(summed, step, 0)
            step *= 2
        counts = jnp.minimum(at + 1, window).astype(jnp.float32)
        pooled = (summed[HALO:] / counts[HALO:] - own[HALO:]).astype(jnp.bfloat16)
        piece = jnp.dot(pooled, pool_ref[group], preferred_element_type=jnp.float32)
        mapped_ref[:, cols] = (piece * scale_ref[:, cols]).astype(jnp.bfloat16)
    mixer = jnp.dot(mapped_ref[...], out_full[...], preferred_element_type=jnp.float32)
    result_ref[...] = (values[HALO:].astype(jnp.float32) + mixer).astype(jnp.bfloat16)


def mix(
    grid, place, values, total, other, mix_gain, inward, pool_weight, pool_scale, outward
):
    rows, width = values.shape[0] - HALO, values.shape[1]
    channels = pool_scale.shape[0]
    whole = pl.BlockSpec(memory_space=pltpu.VMEM)
    return pl.pallas_call(
        functools.partial(mixer_kernel, grid),
        out_shape=jax.ShapeDtypeStruct((rows, width), jnp.bfloat16),
        in_specs=[pl.BlockSpec(memory_space=pltpu.SMEM)] + [whole] * (6 + len(inward) + len(outward)),
        out_specs=whole,
        scratch_shapes=[
            pltpu.VMEM((width, channels), jnp.bfloat16),
            pltpu.VMEM((channels, width), jnp.bfloat16),
            pltpu.VMEM((rows, channels), jnp.bfloat16),
        ],
        cost_estimate=pl.CostEstimate(
            flops=4 * rows * width * channels,
            bytes_accessed=4 * width * channels,
            transcendentals=rows,
        ),
        name="mixer",
    )(
        place, values, total, other, mix_gain[None], *inward, *outward, pool_weight,
        pool_scale[None],
    )


def per_device(
    grid,
    tokens,
    first_gain,
    first_gate,
    first_upward,
    first_down,
    mix_gain,
    mix_input,
    pool_weight,
    pool_scale,
    mix_output,
    second_gain,
    second_gate,
    second_upward,
    second_down,
):
    _, zl, _, x, c = grid.place()
    nx, run = grid.nx, x * CORES + zl
    slots = grid.slots()
    length, part = tokens.shape
    width = part * grid.tp

    near = [
        grid.permute(tokens, lambda zh, zl, y, x, c, k=k: (zh, c ^ k, y, x, zl))
        for k in range(CORES)
    ]
    pieces, places = [], []
    for i in range(nx):
        for k in range(CORES):
            pieces.append(grid.shift_x(near[k], i) if i else near[k])
            places.append((x - i) % nx * CORES + (zl ^ k))
    table = marked(jnp.concatenate([slots, jnp.stack(places).astype(jnp.int32)]))
    row_table = marked(jnp.concatenate([slots, jnp.zeros((1,), jnp.int32)]))
    span_table = jnp.concatenate([slots, x[None].astype(jnp.int32)])

    first_pairs = grid.gather_weight(jnp.concatenate([first_gate, first_upward], 0))
    first_downs = grid.gather_weight(first_down)
    second_pairs = grid.gather_weight(jnp.concatenate([second_gate, second_upward], 0))
    second_downs = grid.gather_weight(second_down)
    inward, outward, mix_table = grid.gather_mixer(mix_input, mix_output)

    chunk = length // CHUNKS
    rows = chunk // grid.tp
    own_before = parts_before = jnp.zeros((HALO, width), jnp.bfloat16)
    firsts, middles, outs = [], [], []
    for h in range(CHUNKS):
        firsts.append(
            hidden_units(table, pieces, (chunk, part), h, 1, first_gain, first_pairs)
        )
    for h, (hidden, own) in enumerate(firsts):
        parts = down_product(row_table, hidden, first_downs)[0]
        parts, own = (
            jnp.concatenate([parts_before, parts], 0),
            jnp.concatenate([own_before, own], 0),
        )
        parts_before, own_before = parts[chunk:], own[chunk:]
        take = lambda i: lax.dynamic_slice(
            parts, ((x + i) % nx * CORES * rows, 0), (CORES * rows + HALO, width)
        )
        total = take(0).astype(jnp.float32)
        for i in range(1, nx):
            total = total + grid.shift_x(take(i), i).astype(jnp.float32)
        half = lax.dynamic_slice(total, ((1 - zl) * rows, 0), (rows + HALO, width))
        other = grid.flip_zl(half.astype(jnp.bfloat16))
        residual = lax.dynamic_slice(own, (run * rows, 0), (rows + HALO, width))
        place = jnp.stack([h * chunk + run * rows, zl] + mix_table).astype(jnp.int32)
        mid_out = mix(
            grid, place, residual, total, other, mix_gain, inward, pool_weight, pool_scale,
            outward,
        )
        near = [mid_out, grid.flip_zl(mid_out)]
        middles.append(
            [grid.shift_x(near[k], i) if i else near[k] for i in range(nx) for k in range(CORES)]
        )

    for pieces in middles:
        hidden, middle = hidden_units(table, pieces, (rows, width), 0, 0, second_gain, second_pairs)
        parts = down_product(span_table, hidden, second_downs, nx)
        span = width // nx
        total = parts[0].astype(jnp.float32)
        for i in range(nx):
            to = lambda zh, c, y, x: (zh, c, y, (x + i) % nx, c)
            if i:
                other = grid.permute(
                    parts[i], lambda zh, zl, y, x, c: to(zh, c, y, x) if zl == c else None
                )
                total = total + other.astype(jnp.float32)
            other = grid.permute(
                parts[i], lambda zh, zl, y, x, c: to(zh, c, y, x) if zl != c else None
            )
            total = total + other.astype(jnp.float32)
        residual = lax.dynamic_slice(middle, (0, x * span), (chunk, span))
        done = (residual.astype(jnp.float32) + 0.5 * total).astype(jnp.bfloat16)
        mine = lax.dynamic_slice(done, (0, c * part), (chunk, part))
        passed = lax.dynamic_slice(done, (0, (1 - c) * part), (chunk, part))
        passed = grid.flip_core(passed)
        outs.append(jnp.where(zl == c, mine, passed))
    return jnp.concatenate(outs, 0)


def solution(mesh):
    in_specs = (
        P("fs", "tp"),
        P(),
        P("fs", "tp"),
        P("fs", "tp"),
        P("tp", "fs"),
        P(),
        P("fs", "tp"),
        P(),
        P(),
        P("tp", "fs"),
        P(),
        P("fs", "tp"),
        P("fs", "tp"),
        P("tp", "fs"),
    )
    grid = Grid(mesh)

    def body(*arrays):
        return per_device(grid, *arrays)

    return jax.shard_map(
        body,
        mesh=mesh,
        in_specs=in_specs,
        out_specs=P("fs", "tp"),
        check_vma=False,
    )
```

```python
import functools
import jax
import jax.numpy as jnp
from jax import lax
from jax.experimental import pallas as pl
from jax.experimental.pallas import tpu as pltpu
from jax.sharding import PartitionSpec as P


GROUP_DIM = 128
EPSILON = 1e-06
HALO = 16
CORES = 2
CHUNKS = 2
AXES = ("fs", "tp")


class Grid:
    def __init__(self, mesh):
        self.fs, self.tp = mesh.shape["fs"], mesh.shape["tp"]
        self.nx = self.tp // CORES
        self.ny = self.nx
        self.nzh = self.fs // (CORES * self.ny)
        self.split = self.nx == self.nzh

    def place(self):
        fs, tp = lax.axis_index("fs"), lax.axis_index("tp")
        y, z = fs % self.ny, fs // self.ny
        return z // CORES, z % CORES, y, tp // CORES, tp % CORES

    def permute(self, value, target):
        pairs, stay = [], False
        for source in range(self.fs * self.tp):
            fs, tp = divmod(source, self.tp)
            z, y = divmod(fs, self.ny)
            to = target(z // CORES, z % CORES, y, tp // CORES, tp % CORES)
            if to is not None:
                zh, zl, y, x, c = to
                goal = ((zh * CORES + zl) * self.ny + y) * self.tp + x * CORES + c
                stay = stay or goal == source
                if goal != source:
                    pairs.append((source, goal))
        moved = lax.ppermute(value, AXES, pairs)
        if stay:
            here = self.place()
            same = [a == b for a, b in zip(target(*here), here)]
            moved = jnp.where(functools.reduce(jnp.logical_and, same), value, moved)
        return moved

    def shift_x(self, value, i):
        return self.permute(value, lambda zh, zl, y, x, c: (zh, zl, y, (x + i) % self.nx, c))

    def shift_y(self, value, j):
        return self.permute(value, lambda zh, zl, y, x, c: (zh, zl, (y + j) % self.ny, x, c))

    def flip_zl(self, value):
        return self.permute(value, lambda zh, zl, y, x, c: (zh, 1 - zl, y, x, c))

    def flip_core(self, value):
        return self.permute(value, lambda zh, zl, y, x, c: (zh, zl, y, x, 1 - c))

    def gather_lines(self, shard):
        return [
            self.permute(shard, lambda zh, zl, y, x, c: ((zh + i) % self.nzh, c, y, x, zl))
            for i in range(self.nzh)
        ]

    def gather_weight(self, shard, near_first=False):
        lines = self.gather_lines(shard)
        if near_first:
            zh, _, _, x, _ = self.place()
            received, lines = lines, []
            for r in range(self.nzh):
                line = received[0]
                for i in range(1, self.nzh):
                    line = jnp.where((zh - x - r) % self.nzh == i, received[i], line)
                lines.append(line)
        planes = list(lines)
        for j in range(1, self.ny):
            for value in lines:
                planes.append(self.shift_y(value, j))
        return planes + [self.flip_core(value) for value in planes]

    def gather_mixer(self, mix_input, mix_output):
        zh, zl, y, x, c = self.place()
        nzh, nx, ny = self.nzh, self.nx, self.ny
        value = joined(self.gather_lines(jnp.stack([mix_input, mix_output])))
        value = joined([value, self.flip_zl(value)])
        inward, outward = value[:, :, 0], value[:, :, 1]
        inward = joined([inward] + [self.shift_y(inward, j) for j in range(1, ny)])
        outward = joined([outward] + [self.shift_x(outward, i) for i in range(1, nx)])
        inward = [inward] + [self.shift_x(inward, i) for i in range(1, nx)]
        outward = [outward] + [self.shift_y(outward, j) for j in range(1, ny)]
        inward += [self.flip_core(v) for v in inward]
        outward += [self.flip_core(v) for v in outward]
        table = [(x - i) % nx for i in range(nx)] + [(y - j) % ny for j in range(ny)]
        table += [(zh - i) % nzh for i in range(nzh)] + [zl, 1 - zl, c, 1 - c]
        return inward, outward, table

    def slots(self, near_first=False):
        zh, _, y, x, c = self.place()
        found = []
        for k in range(CORES):
            for j in range(self.ny):
                for i in range(self.nzh):
                    z = (x + i if near_first else zh - i) % self.nzh
                    z = z * CORES + (c + k) % CORES
                    found.append(z * self.ny + (y - j) % self.ny)
        return jnp.stack(found).astype(jnp.int32)


def joined(pieces):
    return jnp.concatenate([piece[None] for piece in pieces], 0)


def normalize(values, weight_gain):
    wide = values.astype(jnp.float32)
    factor = lax.rsqrt(jnp.mean(wide * wide, axis=-1, keepdims=True) + EPSILON)
    return (wide * factor * weight_gain).astype(jnp.bfloat16)


def hidden_kernel(count, depth, parts, axis, table_ref, gain_ref, *refs):
    pieces, refs = refs[:parts], refs[parts:]
    gates, upwards = refs[:count], refs[count : 2 * count]
    out_ref, values_ref, gate_ref, upward_ref, normed_ref = refs[2 * count :]

    @pl.when(pl.program_id(0) == 0)
    def _():
        for n, piece in enumerate(pieces):
            size = piece.shape[axis]
            start = pl.multiple_of(table_ref[count + n] * size, size)
            if axis:
                values_ref[:, pl.ds(start, size)] = piece[...]
            else:
                values_ref[pl.ds(start, size), :] = piece[...]
        normed_ref[...] = normalize(values_ref[...], gain_ref[...])

    for at in range(count):
        start = pl.multiple_of(table_ref[at] * depth, depth)
        gate_ref[pl.ds(start, depth), :] = gates[at][...]
        upward_ref[pl.ds(start, depth), :] = upwards[at][...]
    values = normed_ref[...]
    gated = jnp.dot(values, gate_ref[...], preferred_element_type=jnp.float32)
    upward = jnp.dot(values, upward_ref[...], preferred_element_type=jnp.float32)
    out_ref[...] = (gated / (1.0 + jnp.exp(-gated)) * upward).astype(jnp.bfloat16)


def hidden_units(table, pieces, piece_shape, piece_row, axis, weight_gain, gates, upwards):
    count, width = len(gates), gates[0].shape[1]
    depth = weight_gain.shape[0]
    stacked = gates[0].shape[0] // (depth // count) - 1
    rows = piece_shape[0] * (1 if axis else len(pieces))
    tile = min(width, 512) if width % 512 == 0 else 256
    block = depth // count
    piece_spec = pl.BlockSpec(piece_shape, lambda j, s: (piece_row, 0))
    gate_spec = pl.BlockSpec((block, tile), lambda j, s: (0, j))
    upward_spec = pl.BlockSpec((block, tile), lambda j, s: (stacked, j))
    return pl.pallas_call(
        functools.partial(hidden_kernel, count, block, len(pieces), axis),
        out_shape=(
            jax.ShapeDtypeStruct((rows, width), jnp.bfloat16),
            jax.ShapeDtypeStruct((rows, depth), jnp.bfloat16),
        ),
        grid_spec=pltpu.PrefetchScalarGridSpec(
            num_scalar_prefetch=1,
            grid=(width // tile,),
            in_specs=[pl.BlockSpec((1, depth), lambda j, s: (0, 0))]
            + [piece_spec] * len(pieces)
            + [gate_spec] * count
            + [upward_spec] * count,
            out_specs=(
                pl.BlockSpec((rows, tile), lambda j, s: (0, j)),
                pl.BlockSpec((rows, depth), lambda j, s: (0, 0)),
            ),
            scratch_shapes=[pltpu.VMEM((depth, tile), jnp.bfloat16)] * 2
            + [pltpu.VMEM((rows, depth), jnp.bfloat16)],
        ),
        cost_estimate=pl.CostEstimate(
            flops=4 * rows * depth * width,
            bytes_accessed=4 * depth * width + 2 * rows * (2 * depth + width),
            transcendentals=rows * width,
        ),
        name="hidden_units",
    )(table, weight_gain[None], *pieces, *gates, *upwards)


def down_kernel(count, width, first, step, slot_ref, hidden_ref, *refs):
    downs, out_ref = refs[:count], refs[count]
    hidden = hidden_ref[...]
    for at in range(count):
        piece = jnp.dot(hidden, downs[at][...], preferred_element_type=jnp.float32)
        start = pl.multiple_of(slot_ref[first + at * step] % count * width, width)
        out_ref[:, pl.ds(start, width)] = piece.astype(jnp.bfloat16)


def down_product(table, hidden, downs, first=0, step=1, tile=256):
    downs = downs[first::step]
    rows, depth = hidden.shape
    count, width = len(downs), downs[0].shape[1]
    return pl.pallas_call(
        functools.partial(down_kernel, count, width, first, step),
        out_shape=jax.ShapeDtypeStruct((rows, count * width), jnp.bfloat16),
        grid_spec=pltpu.PrefetchScalarGridSpec(
            num_scalar_prefetch=1,
            grid=(rows // tile,),
            in_specs=[pl.BlockSpec((tile, depth), lambda j, s: (j, 0))]
            + [pl.BlockSpec((depth, width), lambda j, s: (0, 0))] * count,
            out_specs=pl.BlockSpec((tile, count * width), lambda j, s: (j, 0)),
        ),
        cost_estimate=pl.CostEstimate(
            flops=2 * rows * depth * count * width,
            bytes_accessed=2 * depth * count * width + 2 * rows * (depth + count * width),
            transcendentals=0,
        ),
        name="down_product",
    )(table, hidden, *downs)


def marked(table):
    def copy(source, target):
        for n in range(table.shape[0]):
            target[n] = source[n]

    spec = pl.BlockSpec(memory_space=pltpu.SMEM)
    return pl.pallas_call(
        copy,
        out_shape=jax.ShapeDtypeStruct(table.shape, table.dtype),
        in_specs=[spec],
        out_specs=spec,
        name="mark",
    )(table)


def mixer_kernel(grid, place_ref, values_ref, total_ref, other_ref, gain_ref, *refs):
    nx, ny = grid.nx, grid.ny
    inward, refs = refs[: CORES * nx], refs[CORES * nx :]
    outward, refs = refs[: CORES * ny], refs[CORES * ny :]
    pool_ref, scale_ref, result_ref, in_full, out_full, mapped_ref = refs
    rows = result_ref.shape[0]
    entry = iter(range(2, place_ref.shape[0]))
    xs, ys, zhs, zls, cs = (
        [place_ref[next(entry)] for _ in range(n)] for n in (nx, ny, grid.nzh, CORES, CORES)
    )
    for k, c in enumerate(cs):
        for l, zl in enumerate(zls):
            for m, zh in enumerate(zhs):
                for i, x in enumerate(xs):
                    for j, y in enumerate(ys):
                        model, channel = (zh * CORES + c) * ny + y, x * CORES + zl
                        piece = inward[k * nx + i][j, l, m]
                        at = pl.multiple_of(model * piece.shape[0], piece.shape[0])
                        to = pl.multiple_of(channel * piece.shape[1], piece.shape[1])
                        in_full[pl.ds(at, piece.shape[0]), pl.ds(to, piece.shape[1])] = piece
                        piece = outward[k * ny + j][i, l, m]
                        at = pl.multiple_of(channel * piece.shape[0], piece.shape[0])
                        to = pl.multiple_of(model * piece.shape[1], piece.shape[1])
                        out_full[pl.ds(at, piece.shape[0]), pl.ds(to, piece.shape[1])] = piece
    half = pl.multiple_of(place_ref[1] * rows, rows)
    total = total_ref[pl.ds(half, rows + HALO), :] + other_ref[...].astype(jnp.float32)
    values = (values_ref[...].astype(jnp.float32) + 0.5 * total).astype(jnp.bfloat16)
    pool_in = jnp.dot(
        normalize(values, gain_ref[...]), in_full[...], preferred_element_type=jnp.float32
    )
    pool_in = pool_in.astype(jnp.bfloat16).astype(jnp.float32)
    at = place_ref[0] - HALO + lax.broadcasted_iota(jnp.int32, (rows + HALO, GROUP_DIM), 0)
    for group in range(pool_in.shape[1] // GROUP_DIM):
        cols = slice(group * GROUP_DIM, (group + 1) * GROUP_DIM)
        window = 2 ** (1 + group % 4)
        own = jnp.where(at >= 0, pool_in[:, cols], 0.0)
        summed, step = own, 1
        while step < window:
            summed = summed + pltpu.roll(summed, step, 0)
            step *= 2
        counts = jnp.minimum(at + 1, window).astype(jnp.float32)
        pooled = (summed[HALO:] / counts[HALO:] - own[HALO:]).astype(jnp.bfloat16)
        piece = jnp.dot(pooled, pool_ref[group], preferred_element_type=jnp.float32)
        mapped_ref[:, cols] = (piece * scale_ref[:, cols]).astype(jnp.bfloat16)
    mixer = jnp.dot(mapped_ref[...], out_full[...], preferred_element_type=jnp.float32)
    result_ref[...] = (values[HALO:].astype(jnp.float32) + mixer).astype(jnp.bfloat16)


def mix(
    grid, place, values, total, other, mix_gain, inward, pool_weight, pool_scale, outward
):
    rows, width = values.shape[0] - HALO, values.shape[1]
    channels = pool_scale.shape[0]
    whole = pl.BlockSpec(memory_space=pltpu.VMEM)
    return pl.pallas_call(
        functools.partial(mixer_kernel, grid),
        out_shape=jax.ShapeDtypeStruct((rows, width), jnp.bfloat16),
        in_specs=[pl.BlockSpec(memory_space=pltpu.SMEM)] + [whole] * (6 + len(inward) + len(outward)),
        out_specs=whole,
        scratch_shapes=[
            pltpu.VMEM((width, channels), jnp.bfloat16),
            pltpu.VMEM((channels, width), jnp.bfloat16),
            pltpu.VMEM((rows, channels), jnp.bfloat16),
        ],
        cost_estimate=pl.CostEstimate(
            flops=4 * rows * width * channels,
            bytes_accessed=4 * width * channels,
            transcendentals=rows,
        ),
        name="mixer",
    )(
        place, values, total, other, mix_gain[None], *inward, *outward, pool_weight,
        pool_scale[None],
    )


def per_device(
    grid,
    tokens,
    first_gain,
    first_gate,
    first_upward,
    first_down,
    mix_gain,
    mix_input,
    pool_weight,
    pool_scale,
    mix_output,
    second_gain,
    second_gate,
    second_upward,
    second_down,
):
    _, zl, _, x, c = grid.place()
    nx, run = grid.nx, x * CORES + zl
    slots = grid.slots()
    length, part = tokens.shape
    width = part * grid.tp

    near = [
        grid.permute(tokens, lambda zh, zl, y, x, c, k=k: (zh, c ^ k, y, x, zl))
        for k in range(CORES)
    ]
    pieces, places = [], []
    for i in range(nx):
        for k in range(CORES):
            pieces.append(grid.shift_x(near[k], i) if i else near[k])
            places.append((x - i) % nx * CORES + (zl ^ k))
    table = marked(jnp.concatenate([slots, jnp.stack(places).astype(jnp.int32)]))
    row_table = marked(slots)
    span_table = jnp.concatenate([grid.slots(grid.split), x[None].astype(jnp.int32)])
    span_table = marked(span_table)

    first_gates = grid.gather_weight(first_gate)
    first_upwards = grid.gather_weight(first_upward)
    first_downs = grid.gather_weight(first_down)
    second_pair = jnp.concatenate([second_gate, second_upward], 0)
    second_pairs = grid.gather_weight(second_pair)
    second_downs = grid.gather_weight(second_down, grid.split)
    inward, outward, mix_table = grid.gather_mixer(mix_input, mix_output)

    chunk = length // CHUNKS
    rows = chunk // grid.tp
    own_before = parts_before = jnp.zeros((HALO, width), jnp.bfloat16)
    firsts, middles, outs = [], [], []
    for h in range(CHUNKS):
        firsts.append(
            hidden_units(table, pieces, (chunk, part), h, 1, first_gain, first_gates, first_upwards)
        )
    for h, (hidden, own) in enumerate(firsts):
        parts = down_product(row_table, hidden, first_downs)
        parts, own = (
            jnp.concatenate([parts_before, parts], 0),
            jnp.concatenate([own_before, own], 0),
        )
        parts_before, own_before = parts[chunk:], own[chunk:]
        take = lambda i: lax.dynamic_slice(
            parts, ((x + i) % nx * CORES * rows, 0), (CORES * rows + HALO, width)
        )
        total = take(0).astype(jnp.float32)
        for i in range(1, nx):
            total = total + grid.shift_x(take(i), i).astype(jnp.float32)
        half = lax.dynamic_slice(total, ((1 - zl) * rows, 0), (rows + HALO, width))
        other = grid.flip_zl(half.astype(jnp.bfloat16))
        residual = lax.dynamic_slice(own, (run * rows, 0), (rows + HALO, width))
        place = jnp.stack([h * chunk + run * rows, zl] + mix_table).astype(jnp.int32)
        mid_out = mix(
            grid, place, residual, total, other, mix_gain, inward, pool_weight, pool_scale,
            outward,
        )
        near = [mid_out, grid.flip_zl(mid_out)]
        middles.append(
            [grid.shift_x(near[k], i) if i else near[k] for i in range(nx) for k in range(CORES)]
        )

    span = width // nx
    for pieces in middles:
        hidden, middle = hidden_units(
            table, pieces, (rows, width), 0, 0, second_gain, second_pairs, second_pairs
        )
        parts = []
        for i in range(nx):
            if grid.split:
                parts.append(down_product(span_table, hidden, second_downs, i, nx))
                continue
            if i == 0:
                product = down_product(span_table, hidden, second_downs)
            at = (x + i) % nx * span
            parts.append(lax.dynamic_slice(product, (0, at), (chunk, span)))
        others = []
        for i in range(nx):
            to = lambda zh, c, y, x: (zh, c, y, (x + i) % nx, c)
            if i:
                others.append(
                    grid.permute(
                        parts[i], lambda zh, zl, y, x, c: to(zh, c, y, x) if zl == c else None
                    )
                )
            others.append(
                grid.permute(parts[i], lambda zh, zl, y, x, c: to(zh, c, y, x) if zl != c else None)
            )
        total = parts[0].astype(jnp.float32)
        for other in others:
            total = total + other.astype(jnp.float32)
        residual = lax.dynamic_slice(middle, (0, x * span), (chunk, span))
        done = (residual.astype(jnp.float32) + 0.5 * total).astype(jnp.bfloat16)
        mine = lax.dynamic_slice(done, (0, c * part), (chunk, part))
        passed = lax.dynamic_slice(done, (0, (1 - c) * part), (chunk, part))
        outs.append((mine, grid.flip_core(passed)))
    mine, passed = (jnp.concatenate(some, 0) for some in zip(*outs))
    return jnp.where(zl == c, mine, passed)


def solution(mesh):
    in_specs = (
        P("fs", "tp"),
        P(),
        P("fs", "tp"),
        P("fs", "tp"),
        P("tp", "fs"),
        P(),
        P("fs", "tp"),
        P(),
        P(),
        P("tp", "fs"),
        P(),
        P("fs", "tp"),
        P("fs", "tp"),
        P("tp", "fs"),
    )
    grid = Grid(mesh)

    def body(*arrays):
        return per_device(grid, *arrays)

    return jax.shard_map(
        body,
        mesh=mesh,
        in_specs=in_specs,
        out_specs=P("fs", "tp"),
        check_vma=False,
    )
```
